32 devices in a mesh: sp: 8 (over z, x), dp: 4 (over y, core).
Axes of the slice: x: 2, y: 2, z: 4, core: 2. Of those that a mesh axis runs over, the one named last changes fastest.
Arguments:
- queries: bfloat16 [4, 1024, 2048], P('dp', 'sp'), may hold values from -12 to 12
- key_rows: bfloat16 [4, 1024, 2048], P('dp', 'sp'), may hold values from -12 to 12
- value_rows: bfloat16 [4, 1024, 2048], P('dp', 'sp'), may hold values from -6 to 6
- lambdas: float32 [16], P('sp'), may hold values from 0.3 to 0.8
- head_gain: float32 [128], replicated, may hold values from 0.1 to 1.9
- out_weight: bfloat16 [2048, 2048], replicated, may hold values from -0.125 to 0.125
- residual: bfloat16 [4, 1024, 2048], P('dp', 'sp'), may hold values from -6 to 6
- mixer_gain: float32 [2048], replicated, may hold values from 0.1 to 1.9
- channel_gain: float32 [2048], replicated, may hold values from 0.1 to 1.9
- expert_gain: float32 [2048], replicated, may hold values from 0.1 to 1.9
- routes: int32 [4, 1024, 2], P('dp', 'sp'), may hold values from 0 to 7, all different within a row; in each aligned block of 128 rows (0 to 127, 128 to 255, ..., all dimensions but the last counted through in order) at most 48 rows name the same one
- route_logits: float32 [4, 1024, 2], P('dp', 'sp'), may hold values from -5 to 5
- gate_weight: bfloat16 [8, 2048, 4096], P('sp', None, 'dp'), may hold values from -0.125 to 0.125
- up_weight: bfloat16 [8, 2048, 4096], P('sp', None, 'dp'), may hold values from -0.125 to 0.125
- down_weight: bfloat16 [8, 4096, 2048], P('sp', 'dp'), may hold values from -0.09375 to 0.09375
Outputs:
- updated: bfloat16 [4, 1024, 2048], P('dp', 'sp')
The draws below stay inside these ranges and needn't reach their ends.
Inputs may be any that keep to these rules, and one draw needn't show every extreme that they name: `routes`: among the rows of one device no expert is named by more than 48 rows; in some of these blocks one expert is named by exactly 48.
All inputs are finite; a program needn't handle non-finite values.
Results may differ from the reference program's by a relative error of at most 0.014.
Values may be sent and summed in bfloat16 or wider, within the bound.
A program may use at most 128 MiB of HBM per device.

```python
import math
import jax
import jax.numpy as jnp
import numpy as np
from jax import lax

D = 2048
HEADS = 16
HD = 64
FF = 4096
TOP = 2
TOK_DEV = 128
LEN = 1024
SEQS = 4
EXPERTS = 8
CAP = 48
N_SP = 8
N_DP = 4


def draw_queries(key, part):
    base = jnp.clip(1.32 * jax.random.normal(jax.random.fold_in(key, 1), (SEQS, LEN, HEADS * 2 * HD), jnp.float32), -12.0, 12.0)
    return base.astype(jnp.bfloat16)


def draw_key_rows(key, part):
    base = jnp.clip(1.32 * jax.random.normal(jax.random.fold_in(key, 2), (SEQS, LEN, HEADS * 2 * HD), jnp.float32), -12.0, 12.0)
    return base.astype(jnp.bfloat16)


def block_scale(stream_key, shape, cuts, low, top_value):
    factor_of, own = 1.0, jax.random.fold_in(stream_key, 6)
    for position, parts in cuts:
        steps = jnp.exp(jax.random.uniform(jax.random.fold_in(own, position), (parts,), jnp.float32, low / len(cuts), top_value / len(cuts)))
        factor_of = factor_of * jnp.repeat(steps, shape[position] // parts).reshape([-1 if axis == position else 1 for axis in range(len(shape))])
    return factor_of


def routed_block(rng, own, number, rows, count, top, most, skew):
    ranking = jax.random.permutation(rng, count)
    heavy_load, usual = load_shares(count, rows * top, most, skew, True), load_shares(count, rows * top, most, skew, False)
    places = jnp.arange(count)

    def named(sizes, turn):
        used = int((sizes > 0).sum())
        fixed = max(1, used // 4)
        passed = fixed + (places - fixed + turn * (used - fixed)) % max(1, count - fixed)
        return jnp.zeros((count,), jnp.int32).at[ranking[jnp.where(places < fixed, places, passed)]].set(jnp.asarray(sizes, jnp.int32))

    sizes = jnp.where(number % 4 == 0, named(heavy_load, number // 4), named(usual, number - number // 4 - 1))
    mixed = jax.random.permutation(jax.random.fold_in(own, 3), count)
    giver, receiver = mixed[0:count // 2 * 2:2], mixed[1:count // 2 * 2:2]
    slack = jnp.minimum(sizes[giver] - 1, most - sizes[receiver]) // 2
    slack = jnp.where((giver == ranking[0]) | (receiver == ranking[0]) | (sizes[receiver] == 0), 0, jnp.maximum(slack, 0))
    passed = jax.random.randint(jax.random.fold_in(own, 4), (count // 2,), 0, 1 << 20) % (slack + 1)
    sizes = sizes.at[giver].add(-passed).at[receiver].add(passed)
    labels = jnp.searchsorted(jnp.cumsum(sizes), jnp.arange(rows * top), side="right").astype(jnp.int32)
    table = labels.reshape(top, rows).T
    table = table[jax.random.permutation(jax.random.fold_in(own, 1), rows)]
    turn = jax.random.randint(jax.random.fold_in(own, 2), (rows, 1), 0, top)
    return jnp.take_along_axis(table, (jnp.arange(top)[None, :] + turn) % top, axis=1)


def load_shares(number_of, total, most, lean, full):
    loads = [(1 << 20) // math.isqrt(grade ** lean) + 1 for grade in range(1, number_of + 1)]
    largest = most if full else min(most, max(-(-total // number_of), total * loads[0] // sum(loads)))
    least = 1 if total - largest >= number_of - 1 else 0
    holding, rest = [largest] + [least] * (number_of - 1), total - largest - least * (number_of - 1)
    while rest > 0:
        free = [i for i in range(1, number_of) if holding[i] < largest] or [i for i in range(1, number_of) if holding[i] < most]
        mass, left = sum([loads[i] for i in free]), rest
        for i in free:
            more = min(most - holding[i], max(1, left * loads[i] // mass), rest)
            holding[i] = holding[i] + more
            rest = rest - more
    return np.array(holding)


def scatter_about(key, shape, deviation, reach, pieces=(), kind=jnp.bfloat16):
    values = deviation * jax.random.normal(key, shape, jnp.float32)
    if pieces:
        values = values * block_scale(key, shape, pieces, -0.22, 0.18)
    return jnp.clip(values, -reach, reach).astype(kind)


def setup_inputs(seed: int = 0) -> dict:
    seeds = jax.random.split(jax.random.key(seed), 16)
    queries = draw_queries(jax.random.fold_in(seeds[15], 71), 0)
    key_rows = draw_key_rows(jax.random.fold_in(seeds[15], 71), 0)
    value_rows = scatter_about(seeds[2], (SEQS, LEN, HEADS * 2 * HD), 1.0, 6.0, ((0, 4), (1, 8)))
    lambdas = jnp.clip(0.3 + 0.5 * jax.random.uniform(seeds[3], (HEADS,), jnp.float32) ** block_scale(seeds[3], (HEADS,), ((0, 8),), -0.2, 0.2), 0.3, 0.8)
    head_gain = jnp.clip(1.0 + 0.18 * jax.random.normal(seeds[4], (2 * HD,), jnp.float32), 0.1, 1.9)
    out_weight = scatter_about(seeds[5], (HEADS * 2 * HD, D), (HEADS * 2 * HD) ** -0.5, 0.125)
    residual = scatter_about(seeds[6], (SEQS, LEN, D), 1.0, 6.0, ((0, 4), (1, 8)))
    mixer_gain = jnp.clip(1.0 + 0.18 * jax.random.normal(seeds[7], (D,), jnp.float32), 0.1, 1.9)
    channel_gain = jnp.clip(1.0 + 0.18 * jax.random.normal(seeds[8], (D,), jnp.float32), 0.1, 1.9)
    expert_gain = jnp.clip(1.0 + 0.18 * jax.random.normal(seeds[9], (D,), jnp.float32), 0.1, 1.9)
    routes_keys = jax.random.split(jax.random.fold_in(seeds[10], 1), SEQS * LEN // TOK_DEV)
    routes_turns = jax.random.permutation(jax.random.fold_in(seeds[10], 3), SEQS * LEN // TOK_DEV)
    routes = jax.vmap(lambda own, number: routed_block(jax.random.fold_in(seeds[10], 2), own, number, TOK_DEV, EXPERTS, TOP, CAP, 2))(routes_keys, routes_turns).reshape((SEQS, LEN, TOP))
    route_logits = scatter_about(seeds[11], (SEQS, LEN, TOP), 1.0, 5.0, ((0, 4), (1, 8)), jnp.float32)
    gate_weight = scatter_about(seeds[12], (EXPERTS, D, FF), D ** -0.5, 0.125, ((0, 8), (2, 4)))
    up_weight = scatter_about(seeds[13], (EXPERTS, D, FF), D ** -0.5, 0.125, ((0, 8), (2, 4)))
    down_weight = scatter_about(seeds[14], (EXPERTS, FF, D), FF ** -0.5, 0.09375, ((0, 8), (1, 4)))
    return {"queries": queries, "key_rows": key_rows, "value_rows": value_rows, "lambdas": lambdas, "head_gain": head_gain, "out_weight": out_weight, "residual": residual, "mixer_gain": mixer_gain, "channel_gain": channel_gain, "expert_gain": expert_gain, "routes": routes, "route_logits": route_logits, "gate_weight": gate_weight, "up_weight": up_weight, "down_weight": down_weight}


def rotate(field):
    dim_full = field.shape[-1]
    dim_half = dim_full // 2
    inverse = 1.0 / 10000.0 ** (jnp.arange(0, dim_full, 2, dtype=jnp.float32) / dim_full)
    angles = jnp.arange(field.shape[-4], dtype=jnp.float32)[:, None] * inverse[None, :]
    cosine = jnp.cos(angles)[:, None, None, :]
    sine_table = jnp.sin(angles)[:, None, None, :]
    floats = field.astype(jnp.float32)
    front_part = floats[..., :dim_half]
    second = floats[..., dim_half:]
    turned = jnp.concatenate([front_part * cosine - second * sine_table, second * cosine + front_part * sine_table], axis=-1)
    return turned.astype(jnp.bfloat16)

def rms_scale(values, epsilon):
    return values * lax.rsqrt(lax.optimization_barrier(jnp.mean(values * values, axis=-1, keepdims=True)) + epsilon)

def reference(queries, key_rows, value_rows, lambdas, head_gain, out_weight, residual, mixer_gain, channel_gain, expert_gain, routes, route_logits, gate_weight, up_weight, down_weight):
    seq_count = queries.shape[0]
    length = queries.shape[1]
    query_rot = rotate(queries.reshape(seq_count, length, HEADS, 2, HD))
    keys_rot = rotate(key_rows.reshape(seq_count, length, HEADS, 2, HD))
    query_items = query_rot.transpose(0, 2, 1, 3, 4).reshape(seq_count * HEADS, length, 2, HD)
    key_items = keys_rot.transpose(0, 2, 1, 3, 4).reshape(seq_count * HEADS, length, 2, HD)
    value_items = value_rows.reshape(seq_count, length, HEADS, 2 * HD).transpose(0, 2, 1, 3).reshape(seq_count * HEADS, length, 2 * HD)
    lambda_items = jnp.tile(lambdas, seq_count)

    def one_head(item):
        query_one, key_one, value_one, lambda_one = item
        scores = jnp.einsum('qcd,kcd->cqk', query_one.astype(jnp.float32), key_one.astype(jnp.float32)) * HD ** (-0.5)
        probs = jax.nn.softmax(scores, axis=-1)
        mixing = (probs[0] - lambda_one * probs[1]).astype(jnp.bfloat16)
        head_mix = jnp.dot(mixing, value_one, preferred_element_type=jnp.float32)
        return (rms_scale(head_mix, 1e-05) * head_gain).astype(jnp.bfloat16)
    heads_out = lax.map(one_head, (query_items, key_items, value_items, lambda_items))
    attended = heads_out.reshape(seq_count, HEADS, length, 2 * HD).transpose(0, 2, 1, 3).reshape(seq_count * length, HEADS * 2 * HD)
    projected = jnp.dot(attended, out_weight, preferred_element_type=jnp.float32)
    stream = (residual.reshape(seq_count * length, D).astype(jnp.float32) + rms_scale(projected, 1e-06) * mixer_gain).astype(jnp.bfloat16)
    normed = (rms_scale(stream.astype(jnp.float32), 1e-06) * channel_gain).astype(jnp.bfloat16)
    choice_ids = routes.reshape(-1).astype(jnp.int32)
    token_of = jnp.arange(choice_ids.shape[0], dtype=jnp.int32) // TOP
    shares = jax.nn.softmax(route_logits.reshape(-1, TOP), axis=-1).reshape(-1)
    limit = N_SP * N_DP * CAP
    block_units = FF // N_DP

    def per_expert(total, expert):
        others = (choice_ids != expert).astype(jnp.int32)
        order = jnp.argsort(others, stable=True)[:limit].astype(jnp.int32)
        count = jnp.sum(1 - others)
        valid = (jnp.arange(limit, dtype=jnp.int32) < count).astype(jnp.float32)
        tok_index = token_of[order]
        rows = normed[tok_index]
        gate_act = jnp.dot(rows, gate_weight[expert], preferred_element_type=jnp.float32)
        up_act = jnp.dot(rows, up_weight[expert], preferred_element_type=jnp.float32)
        hidden = (jax.nn.silu(gate_act) * up_act).astype(jnp.bfloat16)
        expert_sum = jnp.zeros((limit, D), jnp.float32)
        for block in range(N_DP):
            part = jnp.dot(hidden[:, block * block_units:(block + 1) * block_units], down_weight[expert, block * block_units:(block + 1) * block_units], preferred_element_type=jnp.float32)
            expert_sum = expert_sum + lax.optimization_barrier(part.astype(jnp.bfloat16)).astype(jnp.float32)
        expert_out = expert_sum.astype(jnp.bfloat16).astype(jnp.float32)
        weighted = expert_out * (shares[order] * valid)[:, None]
        return (total.at[tok_index].add(weighted), None)
    combined, _ = lax.scan(per_expert, jnp.zeros((seq_count * length, D), jnp.float32), jnp.arange(EXPERTS, dtype=jnp.int32))
    updated = stream.astype(jnp.float32) + rms_scale(combined, 1e-06) * expert_gain
    return updated.astype(jnp.bfloat16).reshape(seq_count, length, D)
```

```python
import functools
import math

import jax
import jax.numpy as jnp
from jax import lax
from jax.experimental import pallas as pl
from jax.experimental.pallas import tpu as pltpu
from jax.sharding import PartitionSpec as P


def rotate(field):
    dim_full = field.shape[-1]
    dim_half = dim_full // 2
    inverse = 1.0 / 10000.0 ** (jnp.arange(0, dim_full, 2, dtype=jnp.float32) / dim_full)
    angles = jnp.arange(field.shape[-4], dtype=jnp.float32)[:, None] * inverse[None, :]
    cosine = jnp.cos(angles)[:, None, None, :]
    sine_table = jnp.sin(angles)[:, None, None, :]
    floats = field.astype(jnp.float32)
    front_part = floats[..., :dim_half]
    second = floats[..., dim_half:]
    turned = jnp.concatenate(
        [front_part * cosine - second * sine_table, second * cosine + front_part * sine_table],
        axis=-1,
    )
    return turned.astype(jnp.bfloat16)


def rms_scale(values, epsilon):
    return values * lax.rsqrt(jnp.mean(values * values, axis=-1, keepdims=True) + epsilon)


MESH = pl.DeviceIdType.MESH


def expert_kernel(
    count,
    groups,
    rows_ref,
    place_ref,
    mix_ref,
    stream_ref,
    gain_ref,
    gate_hbm,
    up_hbm,
    down_hbm,
    out_ref,
    outgoing,
    arrived,
    own,
    pair_in,
    cross_in,
    final,
    returned,
    hidden,
    gate_w,
    up_w,
    down_w,
    w_sem,
    a_send,
    a_recv,
    b_send,
    b_recv,
    c_send,
    c_recv,
    d_send,
    d_recv,
    e_send,
    e_recv,
    f_send,
    f_recv,
):
    me = lax.axis_index("sp")
    dp = lax.axis_index("dp")
    chip, core = dp // 2, dp % 2
    other = {"sp": me, "dp": chip * 2 + (1 - core)}

    def chip_at(step):
        return {"sp": me, "dp": ((chip + step + groups) % groups) * 2 + core}

    def sp_at(step):
        return {"sp": (me + step + count) % count, "dp": dp}

    def remote(src, dst, send, recv, device):
        return pltpu.make_async_remote_copy(
            src_ref=src, dst_ref=dst, send_sem=send, recv_sem=recv, device_id=device, device_id_type=MESH
        )

    def send_out(k):
        return remote(outgoing.at[k], arrived.at[k, 0, 0], a_send.at[k], a_recv.at[k], sp_at(k))

    def cross_out(k, j):
        return remote(arrived.at[k, 0, 0], arrived.at[k, 0, j], b_send.at[k, j], b_recv.at[k, j], chip_at(j))

    def twin_out(k, j):
        return remote(arrived.at[k, 0, j], arrived.at[k, 1, j], c_send.at[k, j], c_recv.at[k, j], other)

    def pair_out(k):
        return remote(arrived.at[k, 1], pair_in.at[k], d_send.at[k], d_recv.at[k], other)

    def cross_back(k, j):
        return remote(own.at[k, j], cross_in.at[k, j], e_send.at[k, j], e_recv.at[k, j], chip_at(-j))

    def send_back(k):
        return remote(final.at[k], returned.at[k], f_send.at[k], f_recv.at[k], sp_at(-k))

    weights = [
        pltpu.make_async_copy(hbm, vmem, w_sem.at[i])
        for i, (hbm, vmem) in enumerate(((gate_hbm, gate_w), (up_hbm, up_w), (down_hbm, down_w)))
    ]
    for copy in weights:
        copy.start()

    barrier = pltpu.get_barrier_semaphore()
    peers = [sp_at(k) for k in range(1, count)] + [chip_at(j) for j in range(1, groups)] + [other]
    for peer in peers:
        pl.semaphore_signal(barrier, inc=1, device_id=peer, device_id_type=MESH)

    capacity = outgoing.shape[1]
    model = rows_ref.shape[1]
    units = gate_w.shape[1]
    wide = math.gcd(model, 512)

    @pl.loop(0, model // wide)
    def _(n):
        cols = pl.ds(pl.multiple_of(n * wide, wide), wide)
        block = jnp.dot(place_ref[...], rows_ref[:, cols], preferred_element_type=jnp.float32)
        block = block.astype(jnp.bfloat16).reshape(count, capacity, wide)
        arrived[0, 0, 0, :, cols] = block[0]
        outgoing[:, :, cols] = block

    pl.semaphore_wait(barrier, len(peers))

    @pl.loop(1, count)
    def _(k):
        send_out(k).start()

    width = 2
    rounds = count // width

    def per_k(group, action):
        for i in range(width):
            action(group * width + i)

    def forward(k):
        @pl.when(k > 0)
        def _():
            send_out(k).wait_recv()

        for j in range(1, groups):
            cross_out(k, j).start()
        twin_out(k, 0).start()

    def forward_twin(k):
        for j in range(1, groups):
            cross_out(k, j).wait_recv()
            twin_out(k, j).start()

    def complete(k):
        for j in range(groups):
            twin_out(k, j).wait_recv()

    def pair_sum(k):
        pair_out(k).wait_recv()
        for j in range(groups):
            own[k, j] = (own[k, j].astype(jnp.float32) + pair_in[k, j].astype(jnp.float32)).astype(jnp.bfloat16)
        for j in range(1, groups):
            cross_back(k, j).start()

    def total(k):
        value = own[k, 0].astype(jnp.float32)
        for j in range(1, groups):
            cross_back(k, j).wait_recv()
            value = value + cross_in[k, j].astype(jnp.float32)
        value = value.astype(jnp.bfloat16)

        @pl.when(k > 0)
        def _():
            final[k] = value
            send_back(k).start()

        @pl.when(k == 0)
        def _():
            returned[k] = value

    tile = math.gcd(units, 256)

    def compute(group):
        first = group * width
        held = width * 2 * groups * capacity
        slab = arrived.at[pl.ds(first, width)]

        @pl.loop(0, units // tile)
        def _(n):
            cols = pl.ds(pl.multiple_of(n * tile, tile), tile)
            value = slab[...].reshape(held, model)
            gate = jnp.dot(value, gate_w[:, cols], preferred_element_type=jnp.float32)
            up = jnp.dot(value, up_w[:, cols], preferred_element_type=jnp.float32)
            hidden[:, cols] = (gate / (1.0 + jnp.exp(-gate)) * up).astype(jnp.bfloat16)

        @pl.loop(0, model // wide)
        def _(n):
            cols = pl.ds(pl.multiple_of(n * wide, wide), wide)
            part = jnp.dot(hidden[...], down_w[:, cols], preferred_element_type=jnp.float32)
            part = part.astype(jnp.bfloat16).reshape(width, 2, groups, capacity, wide)
            for i in range(width):
                own[first + i, :, :, cols] = part[i, 0]
                arrived[first + i, 1, :, :, cols] = part[i, 1]

        per_k(group, lambda k: pair_out(k).start())

    @pl.loop(0, rounds + 3)
    def _(g):
        @pl.when(g < rounds)
        def _():
            per_k(g, forward)

        @pl.when((g >= 2) & (g < rounds + 2))
        def _():
            per_k(g - 2, pair_sum)

        @pl.when(g >= 3)
        def _():
            per_k(g - 3, total)

        @pl.when((g >= 1) & (g < rounds + 1))
        def _():
            @pl.when(g == 1)
            def _():
                for copy in weights:
                    copy.wait()

            per_k(g - 1, forward_twin)
            per_k(g - 1, complete)
            compute(g - 1)

    @pl.loop(1, count)
    def _(k):
        send_back(k).wait_recv()

    square = jnp.zeros((stream_ref.shape[0], 1), jnp.float32)
    share = mix_ref[...]
    high = share.astype(jnp.bfloat16)
    low = (share - high.astype(jnp.float32)).astype(jnp.bfloat16)
    pieces = []
    for n in range(model // wide):
        cols = slice(n * wide, (n + 1) * wide)
        back = returned[:, :, cols].reshape(count * capacity, wide)
        piece = jnp.dot(high, back, preferred_element_type=jnp.float32)
        piece = piece + jnp.dot(low, back, preferred_element_type=jnp.float32)
        square = square + jnp.sum(piece * piece, axis=-1, keepdims=True)
        pieces.append(piece)
    norm = lax.rsqrt(square / model + 1e-06)
    for n, piece in enumerate(pieces):
        cols = slice(n * wide, (n + 1) * wide)
        value = stream_ref[:, cols].astype(jnp.float32) + piece * norm * gain_ref[:, cols]
        out_ref[:, cols] = value.astype(jnp.bfloat16)

    @pl.loop(0, count)
    def _(k):
        @pl.when(k > 0)
        def _():
            send_out(k).wait_send()
            send_back(k).wait_send()

        for j in range(1, groups):
            cross_out(k, j).wait_send()
            cross_back(k, j).wait_send()
        for j in range(groups):
            twin_out(k, j).wait_send()
        pair_out(k).wait_send()


def expert_stage(normed, stream, routes, logits, expert_gain, gate_weight, up_weight, down_weight):
    count, dp_count = lax.axis_size("sp"), lax.axis_size("dp")
    groups = dp_count // 2
    tokens, model = normed.shape
    units = gate_weight.shape[1]
    top = routes.shape[1]
    capacity = -(-max(2, 3 * tokens // count) // 16) * 16
    relative = (routes - lax.axis_index("sp") + count) % count
    flat = relative.reshape(-1)
    one_hot = (flat[:, None] == jnp.arange(count, dtype=jnp.int32)[None, :]).astype(jnp.float32)
    slots = tokens * top
    lower = (jnp.arange(slots)[:, None] >= jnp.arange(slots)[None, :]).astype(jnp.float32)
    running = jnp.dot(lower, one_hot, preferred_element_type=jnp.float32)
    slot = jnp.sum(one_hot * running, axis=1).astype(jnp.int32) - 1
    target = (flat * capacity + slot).reshape(tokens, top)
    shares = jax.nn.softmax(logits, axis=-1)
    places = jnp.arange(count * capacity, dtype=jnp.int32)
    mix = jnp.zeros((tokens, count * capacity), jnp.float32)
    place = jnp.zeros((count * capacity, tokens), jnp.bool_)
    for i in range(top):
        mix = mix + jnp.where(target[:, i, None] == places[None, :], shares[:, i, None], 0.0)
        place = place | (target[None, :, i] == places[:, None])
    place = place.astype(jnp.bfloat16)
    vmem, anywhere = pl.BlockSpec(memory_space=pltpu.VMEM), pl.BlockSpec(memory_space=pl.ANY)
    half = jnp.bfloat16
    dma = pltpu.SemaphoreType.DMA
    return pl.pallas_call(
        functools.partial(expert_kernel, count, groups),
        out_shape=jax.ShapeDtypeStruct((tokens, model), jnp.bfloat16),
        in_specs=[vmem] * 5 + [anywhere] * 3,
        out_specs=vmem,
        scratch_shapes=[
            pltpu.VMEM((count, capacity, model), half),
            pltpu.VMEM((count, 2, groups, capacity, model), half),
            pltpu.VMEM((count, groups, capacity, model), half),
            pltpu.VMEM((count, groups, capacity, model), half),
            pltpu.VMEM((count, groups, capacity, model), half),
            pltpu.VMEM((count, capacity, model), half),
            pltpu.VMEM((count, capacity, model), half),
            pltpu.VMEM((4 * groups * capacity, units), half),
            pltpu.VMEM((model, units), half),
            pltpu.VMEM((model, units), half),
            pltpu.VMEM((units, model), half),
            dma((3,)),
            dma((count,)),
            dma((count,)),
            dma((count, groups)),
            dma((count, groups)),
            dma((count, groups)),
            dma((count, groups)),
            dma((count,)),
            dma((count,)),
            dma((count, groups)),
            dma((count, groups)),
            dma((count,)),
            dma((count,)),
        ],
        compiler_params=pltpu.CompilerParams(
            collective_id=1, has_side_effects=True, vmem_limit_bytes=67043328
        ),
        name="experts",
    )(normed, place, mix, stream, expert_gain[None, :], gate_weight, up_weight, down_weight)


def local(
    queries,
    key_rows,
    value_rows,
    lambdas,
    head_gain,
    out_weight,
    residual,
    mixer_gain,
    channel_gain,
    expert_gain,
    routes,
    route_logits,
    gate_weight,
    up_weight,
    down_weight,
):
    head_count = lambdas.shape[0]
    head_dim = head_gain.shape[0] // 2
    seq_query, seq_keys, seq_values = (
        lax.all_to_all(queries, "sp", split_axis=2, concat_axis=1, tiled=True),
        lax.all_to_all(key_rows, "sp", split_axis=2, concat_axis=1, tiled=True),
        lax.all_to_all(value_rows, "sp", split_axis=2, concat_axis=1, tiled=True),
    )
    length = seq_query.shape[1]
    query_rot = rotate(seq_query.reshape(length, head_count, 2, head_dim))
    keys_rot = rotate(seq_keys.reshape(length, head_count, 2, head_dim))
    values_heads = seq_values.reshape(length, head_count, 2 * head_dim)
    block_rows = math.gcd(length, 256)
    query_blocks = query_rot.reshape(length // block_rows, block_rows, head_count, 2, head_dim)
    scale = head_dim ** (-0.5)

    def one_block(query_block):
        scores = (
            jnp.einsum("qhcd,khcd->hcqk", query_block, keys_rot, preferred_element_type=jnp.float32)
            * scale
        )
        probs = jax.nn.softmax(scores, axis=-1)
        mixing = (probs[:, 0] - lambdas[:, None, None] * probs[:, 1]).astype(jnp.bfloat16)
        head_mix = jnp.einsum(
            "hqk,khv->qhv", mixing, values_heads, preferred_element_type=jnp.float32
        )
        return (rms_scale(head_mix, 1e-05) * head_gain).astype(jnp.bfloat16)

    head_out = lax.map(one_block, query_blocks).reshape(1, length, head_count * 2 * head_dim)
    token_rows = lax.all_to_all(head_out, "sp", split_axis=1, concat_axis=2, tiled=True)
    tokens = residual.shape[1]
    model_dim = residual.shape[2]
    projected = jnp.dot(
        token_rows.reshape(tokens, -1), out_weight, preferred_element_type=jnp.float32
    )
    stream = (
        residual.reshape(tokens, model_dim).astype(jnp.float32)
        + rms_scale(projected, 1e-06) * mixer_gain
    ).astype(jnp.bfloat16)
    normed = (rms_scale(stream.astype(jnp.float32), 1e-06) * channel_gain).astype(jnp.bfloat16)
    updated = expert_stage(
        normed,
        stream,
        routes.reshape(tokens, -1),
        route_logits.reshape(tokens, -1),
        expert_gain,
        gate_weight[0],
        up_weight[0],
        down_weight[0],
    )
    return updated.reshape(1, tokens, model_dim)


def solution(mesh):
    placed = (
        P("dp", "sp", None),
        P("dp", "sp", None),
        P("dp", "sp", None),
        P("sp"),
        P(),
        P(),
        P("dp", "sp", None),
        P(),
        P(),
        P(),
        P("dp", "sp", None),
        P("dp", "sp", None),
        P("sp", None, "dp"),
        P("sp", None, "dp"),
        P("sp", "dp", None),
    )
    return jax.shard_map(
        local, mesh=mesh, in_specs=placed, out_specs=P("dp", "sp", None), check_vma=False
    )
```

```python
import functools
import math

import jax
import jax.numpy as jnp
from jax import lax
from jax.experimental import pallas as pl
from jax.experimental.pallas import tpu as pltpu
from jax.sharding import PartitionSpec as P


MESH = pl.DeviceIdType.MESH


def rms_scale(values, epsilon):
    return values * lax.rsqrt(jnp.mean(values * values, axis=-1, keepdims=True) + epsilon)


def attention_kernel(
    count,
    heads,
    query_ref,
    key_ref,
    value_ref,
    cos_ref,
    sin_ref,
    lambda_ref,
    head_gain_ref,
    residual_ref,
    mixer_gain_ref,
    channel_gain_ref,
    weight_hbm,
    stream_ref,
    normed_ref,
    query_out,
    key_out,
    query_in,
    key_in,
    value_in,
    head_out,
    token_rows,
    projected,
    weight,
    w_sem,
    in_send,
    in_recv,
    out_send,
    out_recv,
):
    me = lax.axis_index("sp")
    tokens, model = query_ref.shape
    lanes = head_gain_ref.shape[1]
    map_dim = lanes // 2
    scale = map_dim ** (-0.5)
    load = pltpu.make_async_copy(weight_hbm, weight, w_sem)
    load.start()

    def sp_at(step):
        return {"sp": (me + step + count) % count}

    def columns(owner, h):
        return pl.ds(pl.multiple_of((owner * heads + h) * lanes, lanes), lanes)

    def dest_columns(k, h):
        return columns((me + k) % count, h)

    def remote(src, dst, send, recv, step):
        return pltpu.make_async_remote_copy(
            src_ref=src,
            dst_ref=dst,
            send_sem=send,
            recv_sem=recv,
            device_id=sp_at(step),
            device_id_type=MESH,
        )

    def inward(h, k, i):
        sources = (value_ref.at[:, dest_columns(k, h)], query_out.at[h, k], key_out.at[h, k])
        targets = (value_in.at[h, k], query_in.at[h, k], key_in.at[h, k])
        return remote(sources[i], targets[i], in_send.at[h, i, k], in_recv.at[h, i, k], k)

    def outward(h, k):
        return remote(
            head_out.at[h, k], token_rows.at[:, columns(me, h)], out_send.at[h, k], out_recv.at[h, k], -k
        )

    barrier = pltpu.get_barrier_semaphore()
    for k in range(1, count):
        pl.semaphore_signal(barrier, inc=1, device_id=sp_at(k), device_id_type=MESH)

    first_half = lax.broadcasted_iota(jnp.int32, (tokens, lanes), 1) % map_dim < map_dim // 2

    def turned(ref, cols):
        x = ref[:, cols].astype(jnp.float32)
        ahead = pltpu.roll(x, lanes - map_dim // 2, 1)
        behind = pltpu.roll(x, map_dim // 2, 1)
        return x * cos_ref[...] + jnp.where(first_half, ahead, behind) * sin_ref[...]

    def prepare(h, k):
        cols = dest_columns(k, h)
        query = (turned(query_ref, cols) * scale).astype(jnp.bfloat16)
        key = turned(key_ref, cols).astype(jnp.bfloat16)
        return query, key

    for h in range(heads):
        query, key = prepare(h, 0)
        query_in[h, 0] = query
        key_in[h, 0] = key
        value_in[h, 0] = value_ref[:, columns(me, h)]

    pl.semaphore_wait(barrier, count - 1)

    for h in range(heads):

        @pl.loop(1, count)
        def _(k):
            inward(h, k, 0).start()

        @pl.loop(1, count)
        def _(k):
            query_out[h, k], key_out[h, k] = prepare(h, k)

        @pl.loop(1, count)
        def _(k):
            inward(h, k, 1).start()
            inward(h, k, 2).start()

    width = 2
    rows = width * tokens
    length = count * tokens
    in_first = lax.broadcasted_iota(jnp.int32, (rows, lanes), 1) < map_dim

    def part_of(total):
        return jnp.exp(total - jnp.max(total, axis=-1, keepdims=True))

    for h in range(heads):

        @pl.loop(1, count)
        def _(k):
            for i in range(3):
                inward(h, k, i).wait_recv()

        @pl.loop(0, count // width)
        def _(b):
            query = query_in[h, pl.ds(b * width, width)].reshape(rows, lanes).astype(jnp.float32)
            both = jnp.concatenate(
                [jnp.where(in_first, query, 0.0), jnp.where(in_first, 0.0, query)], axis=0
            ).astype(jnp.bfloat16)
            keys = key_in[h].reshape(length, lanes)
            scores = lax.dot_general(
                both, keys, (((1,), (1,)), ((), ())), preferred_element_type=jnp.float32
            )
            one, two = part_of(scores[:rows]), part_of(scores[rows:])
            one_scale = 1.0 / jnp.sum(one, axis=-1, keepdims=True)
            two_scale = lambda_ref[h] / jnp.sum(two, axis=-1, keepdims=True)
            mixing = (one * one_scale - two * two_scale).astype(jnp.bfloat16)
            mix = jnp.dot(
                mixing, value_in[h].reshape(length, lanes), preferred_element_type=jnp.float32
            )
            result = (rms_scale(mix, 1e-05) * head_gain_ref[...]).astype(jnp.bfloat16)
            head_out[h, pl.ds(b * width, width)] = result.reshape(width, tokens, lanes)
            for i in range(width):
                k = b * width + i

                @pl.when(k > 0)
                def _():
                    outward(h, k).start()

    for h in range(heads):
        token_rows[:, columns(me, h)] = head_out[h, 0]

    load.wait()
    for h in range(heads):

        @pl.loop(1, count)
        def _(k):
            outward(h, k).wait_recv()

    wide = math.gcd(model, 512)

    @pl.loop(0, model // wide)
    def _(n):
        cols = pl.ds(pl.multiple_of(n * wide, wide), wide)
        projected[:, cols] = jnp.dot(
            token_rows[...], weight[:, cols], preferred_element_type=jnp.float32
        )

    chunk = math.gcd(tokens, 16)

    @pl.loop(0, tokens // chunk)
    def _(n):
        part = pl.ds(pl.multiple_of(n * chunk, chunk), chunk)
        stream = residual_ref[part, :].astype(jnp.float32)
        stream = stream + rms_scale(projected[part, :], 1e-06) * mixer_gain_ref[...]
        stream = stream.astype(jnp.bfloat16)
        stream_ref[part, :] = stream
        normed = rms_scale(stream.astype(jnp.float32), 1e-06) * channel_gain_ref[...]
        normed_ref[part, :] = normed.astype(jnp.bfloat16)

    for h in range(heads):

        @pl.loop(1, count)
        def _(k):
            for i in range(3):
                inward(h, k, i).wait_send()
            outward(h, k).wait_send()


def attention_stage(
    queries, keys, values, lambdas, head_gain, out_weight, residual, mixer_gain, channel_gain
):
    count = lax.axis_size("sp")
    heads = lambdas.shape[0]
    lanes = head_gain.shape[0]
    map_dim = lanes // 2
    tokens, model = residual.shape
    inverse = 1.0 / 10000.0 ** (jnp.arange(0, map_dim, 2, dtype=jnp.float32) / map_dim)
    positions = lax.axis_index("sp") * tokens + jnp.arange(tokens, dtype=jnp.int32)
    angles = positions.astype(jnp.float32)[:, None] * inverse[None, :]
    cosine, sine = jnp.cos(angles), jnp.sin(angles)
    cos_table = jnp.concatenate([cosine] * 4, axis=1)
    sin_table = jnp.concatenate([-sine, sine] * 2, axis=1)
    vmem = pl.BlockSpec(memory_space=pltpu.VMEM)
    smem = pl.BlockSpec(memory_space=pltpu.SMEM)
    half = jnp.bfloat16
    dma = pltpu.SemaphoreType.DMA
    blocks = pltpu.VMEM((heads, count, tokens, lanes), half)
    shape = jax.ShapeDtypeStruct((tokens, model), half)
    return pl.pallas_call(
        functools.partial(attention_kernel, count, heads),
        out_shape=[shape, shape],
        in_specs=[vmem] * 5 + [smem] + [vmem] * 4 + [pl.BlockSpec(memory_space=pl.ANY)],
        out_specs=[vmem, vmem],
        scratch_shapes=[
            blocks,
            blocks,
            blocks,
            blocks,
            blocks,
            blocks,
            pltpu.VMEM((tokens, heads * count * lanes), half),
            pltpu.VMEM((tokens, model), jnp.float32),
            pltpu.VMEM(out_weight.shape, half),
            dma,
            dma((heads, 3, count)),
            dma((heads, 3, count)),
            dma((heads, count)),
            dma((heads, count)),
        ],
        compiler_params=pltpu.CompilerParams(
            collective_id=2, has_side_effects=True, vmem_limit_bytes=60 * 1024 * 1024
        ),
        name="attention",
    )(
        queries,
        keys,
        values,
        cos_table,
        sin_table,
        lambdas,
        head_gain[None, :],
        residual,
        mixer_gain[None, :],
        channel_gain[None, :],
        out_weight,
    )


def expert_kernel(
    count,
    groups,
    rows_ref,
    place_ref,
    mix_ref,
    stream_ref,
    gain_ref,
    gate_hbm,
    up_hbm,
    down_hbm,
    out_ref,
    outgoing,
    arrived,
    own,
    pair_in,
    cross_in,
    final,
    returned,
    hidden,
    gate_w,
    up_w,
    down_w,
    w_sem,
    a_send,
    a_recv,
    b_send,
    b_recv,
    c_send,
    c_recv,
    d_send,
    d_recv,
    e_send,
    e_recv,
    f_send,
    f_recv,
):
    me = lax.axis_index("sp")
    dp = lax.axis_index("dp")
    chip, core = dp // 2, dp % 2
    other = {"sp": me, "dp": chip * 2 + (1 - core)}

    def chip_at(step):
        return {"sp": me, "dp": ((chip + step + groups) % groups) * 2 + core}

    def sp_at(step):
        return {"sp": (me + step + count) % count, "dp": dp}

    def remote(src, dst, send, recv, device):
        return pltpu.make_async_remote_copy(
            src_ref=src, dst_ref=dst, send_sem=send, recv_sem=recv, device_id=device, device_id_type=MESH
        )

    def send_out(k):
        return remote(outgoing.at[k], arrived.at[k, 0, 0], a_send.at[k], a_recv.at[k], sp_at(k))

    def cross_out(k, j):
        return remote(arrived.at[k, 0, 0], arrived.at[k, 0, j], b_send.at[k, j], b_recv.at[k, j], chip_at(j))

    def twin_out(k, j):
        return remote(arrived.at[k, 0, j], arrived.at[k, 1, j], c_send.at[k, j], c_recv.at[k, j], other)

    def pair_out(k):
        return remote(arrived.at[k, 1], pair_in.at[k], d_send.at[k], d_recv.at[k], other)

    def cross_back(k, j):
        return remote(own.at[k, j], cross_in.at[k, j], e_send.at[k, j], e_recv.at[k, j], chip_at(-j))

    def send_back(k):
        return remote(final.at[k], returned.at[k], f_send.at[k], f_recv.at[k], sp_at(-k))

    weights = [
        pltpu.make_async_copy(hbm, vmem, w_sem.at[i])
        for i, (hbm, vmem) in enumerate(((gate_hbm, gate_w), (up_hbm, up_w), (down_hbm, down_w)))
    ]
    for copy in weights:
        copy.start()

    barrier = pltpu.get_barrier_semaphore()
    peers = [sp_at(k) for k in range(1, count)] + [chip_at(j) for j in range(1, groups)] + [other]
    for peer in peers:
        pl.semaphore_signal(barrier, inc=1, device_id=peer, device_id_type=MESH)

    capacity = outgoing.shape[1]
    model = rows_ref.shape[1]
    units = gate_w.shape[1]
    wide = math.gcd(model, 512)

    @pl.loop(0, model // wide)
    def _(n):
        cols = pl.ds(pl.multiple_of(n * wide, wide), wide)
        block = jnp.dot(place_ref[...], rows_ref[:, cols], preferred_element_type=jnp.float32)
        block = block.astype(jnp.bfloat16).reshape(count, capacity, wide)
        arrived[0, 0, 0, :, cols] = block[0]
        outgoing[:, :, cols] = block

    pl.semaphore_wait(barrier, len(peers))

    @pl.loop(1, count)
    def _(k):
        send_out(k).start()

    width = 2
    rounds = count // width

    def per_k(group, action):
        for i in range(width):
            action(group * width + i)

    def forward(k):
        @pl.when(k > 0)
        def _():
            send_out(k).wait_recv()

        for j in range(1, groups):
            cross_out(k, j).start()
        twin_out(k, 0).start()

    def forward_twin(k):
        for j in range(1, groups):
            cross_out(k, j).wait_recv()
            twin_out(k, j).start()

    def complete(k):
        for j in range(groups):
            twin_out(k, j).wait_recv()

    def pair_sum(k):
        pair_out(k).wait_recv()
        for j in range(groups):
            own[k, j] = (own[k, j].astype(jnp.float32) + pair_in[k, j].astype(jnp.float32)).astype(jnp.bfloat16)
        for j in range(1, groups):
            cross_back(k, j).start()

    def total(k):
        value = own[k, 0].astype(jnp.float32)
        for j in range(1, groups):
            cross_back(k, j).wait_recv()
            value = value + cross_in[k, j].astype(jnp.float32)
        value = value.astype(jnp.bfloat16)

        @pl.when(k > 0)
        def _():
            final[k] = value
            send_back(k).start()

        @pl.when(k == 0)
        def _():
            returned[k] = value

    tile = math.gcd(units, 256)

    def compute(group):
        first = group * width
        held = width * 2 * groups * capacity
        slab = arrived.at[pl.ds(first, width)]

        @pl.loop(0, units // tile)
        def _(n):
            cols = pl.ds(pl.multiple_of(n * tile, tile), tile)
            value = slab[...].reshape(held, model)
            gate = jnp.dot(value, gate_w[:, cols], preferred_element_type=jnp.float32)
            up = jnp.dot(value, up_w[:, cols], preferred_element_type=jnp.float32)
            hidden[:, cols] = (gate / (1.0 + jnp.exp(-gate)) * up).astype(jnp.bfloat16)

        @pl.loop(0, model // wide)
        def _(n):
            cols = pl.ds(pl.multiple_of(n * wide, wide), wide)
            part = jnp.dot(hidden[...], down_w[:, cols], preferred_element_type=jnp.float32)
            part = part.astype(jnp.bfloat16).reshape(width, 2, groups, capacity, wide)
            for i in range(width):
                own[first + i, :, :, cols] = part[i, 0]
                arrived[first + i, 1, :, :, cols] = part[i, 1]

        per_k(group, lambda k: pair_out(k).start())

    @pl.loop(0, rounds + 3)
    def _(g):
        @pl.when(g < rounds)
        def _():
            per_k(g, forward)

        @pl.when((g >= 2) & (g < rounds + 2))
        def _():
            per_k(g - 2, pair_sum)

        @pl.when(g >= 3)
        def _():
            per_k(g - 3, total)

        @pl.when((g >= 1) & (g < rounds + 1))
        def _():
            @pl.when(g == 1)
            def _():
                for copy in weights:
                    copy.wait()

            per_k(g - 1, forward_twin)
            per_k(g - 1, complete)
            compute(g - 1)

    @pl.loop(1, count)
    def _(k):
        send_back(k).wait_recv()

    square = jnp.zeros((stream_ref.shape[0], 1), jnp.float32)
    share = mix_ref[...]
    high = share.astype(jnp.bfloat16)
    low = (share - high.astype(jnp.float32)).astype(jnp.bfloat16)
    pieces = []
    for n in range(model // wide):
        cols = slice(n * wide, (n + 1) * wide)
        back = returned[:, :, cols].reshape(count * capacity, wide)
        piece = jnp.dot(high, back, preferred_element_type=jnp.float32)
        piece = piece + jnp.dot(low, back, preferred_element_type=jnp.float32)
        square = square + jnp.sum(piece * piece, axis=-1, keepdims=True)
        pieces.append(piece)
    norm = lax.rsqrt(square / model + 1e-06)
    for n, piece in enumerate(pieces):
        cols = slice(n * wide, (n + 1) * wide)
        value = stream_ref[:, cols].astype(jnp.float32) + piece * norm * gain_ref[:, cols]
        out_ref[:, cols] = value.astype(jnp.bfloat16)

    @pl.loop(0, count)
    def _(k):
        @pl.when(k > 0)
        def _():
            send_out(k).wait_send()
            send_back(k).wait_send()

        for j in range(1, groups):
            cross_out(k, j).wait_send()
            cross_back(k, j).wait_send()
        for j in range(groups):
            twin_out(k, j).wait_send()
        pair_out(k).wait_send()


def expert_stage(normed, stream, routes, logits, expert_gain, gate_weight, up_weight, down_weight):
    count, dp_count = lax.axis_size("sp"), lax.axis_size("dp")
    groups = dp_count // 2
    tokens, model = normed.shape
    units = gate_weight.shape[1]
    top = routes.shape[1]
    capacity = -(-max(2, 3 * tokens // count) // 16) * 16
    relative = (routes - lax.axis_index("sp") + count) % count
    flat = relative.reshape(-1)
    one_hot = (flat[:, None] == jnp.arange(count, dtype=jnp.int32)[None, :]).astype(jnp.float32)
    slots = tokens * top
    lower = (jnp.arange(slots)[:, None] >= jnp.arange(slots)[None, :]).astype(jnp.float32)
    running = jnp.dot(lower, one_hot, preferred_element_type=jnp.float32)
    slot = jnp.sum(one_hot * running, axis=1).astype(jnp.int32) - 1
    target = (flat * capacity + slot).reshape(tokens, top)
    shares = jax.nn.softmax(logits, axis=-1)
    places = jnp.arange(count * capacity, dtype=jnp.int32)
    mix = jnp.zeros((tokens, count * capacity), jnp.float32)
    place = jnp.zeros((count * capacity, tokens), jnp.bool_)
    for i in range(top):
        mix = mix + jnp.where(target[:, i, None] == places[None, :], shares[:, i, None], 0.0)
        place = place | (target[None, :, i] == places[:, None])
    place = place.astype(jnp.bfloat16)
    vmem, anywhere = pl.BlockSpec(memory_space=pltpu.VMEM), pl.BlockSpec(memory_space=pl.ANY)
    half = jnp.bfloat16
    dma = pltpu.SemaphoreType.DMA
    return pl.pallas_call(
        functools.partial(expert_kernel, count, groups),
        out_shape=jax.ShapeDtypeStruct((tokens, model), jnp.bfloat16),
        in_specs=[vmem] * 5 + [anywhere] * 3,
        out_specs=vmem,
        scratch_shapes=[
            pltpu.VMEM((count, capacity, model), half),
            pltpu.VMEM((count, 2, groups, capacity, model), half),
            pltpu.VMEM((count, groups, capacity, model), half),
            pltpu.VMEM((count, groups, capacity, model), half),
            pltpu.VMEM((count, groups, capacity, model), half),
            pltpu.VMEM((count, capacity, model), half),
            pltpu.VMEM((count, capacity, model), half),
            pltpu.VMEM((4 * groups * capacity, units), half),
            pltpu.VMEM((model, units), half),
            pltpu.VMEM((model, units), half),
            pltpu.VMEM((units, model), half),
            dma((3,)),
            dma((count,)),
            dma((count,)),
            dma((count, groups)),
            dma((count, groups)),
            dma((count, groups)),
            dma((count, groups)),
            dma((count,)),
            dma((count,)),
            dma((count, groups)),
            dma((count, groups)),
            dma((count,)),
            dma((count,)),
        ],
        compiler_params=pltpu.CompilerParams(
            collective_id=1, has_side_effects=True, vmem_limit_bytes=67043328
        ),
        name="experts",
    )(normed, place, mix, stream, expert_gain[None, :], gate_weight, up_weight, down_weight)


def local(
    queries,
    key_rows,
    value_rows,
    lambdas,
    head_gain,
    out_weight,
    residual,
    mixer_gain,
    channel_gain,
    expert_gain,
    routes,
    route_logits,
    gate_weight,
    up_weight,
    down_weight,
):
    stream, normed = attention_stage(
        queries[0],
        key_rows[0],
        value_rows[0],
        lambdas,
        head_gain,
        out_weight,
        residual[0],
        mixer_gain,
        channel_gain,
    )
    updated = expert_stage(
        normed,
        stream,
        routes[0],
        route_logits[0],
        expert_gain,
        gate_weight[0],
        up_weight[0],
        down_weight[0],
    )
    return updated[None]


def solution(mesh):
    placed = (
        P("dp", "sp", None),
        P("dp", "sp", None),
        P("dp", "sp", None),
        P("sp"),
        P(),
        P(),
        P("dp", "sp", None),
        P(),
        P(),
        P(),
        P("dp", "sp", None),
        P("dp", "sp", None),
        P("sp", None, "dp"),
        P("sp", None, "dp"),
        P("sp", "dp", None),
    )
    return jax.shard_map(
        local, mesh=mesh, in_specs=placed, out_specs=P("dp", "sp", None), check_vma=False
    )
```

```python
import functools
import math

import jax
import jax.numpy as jnp
from jax import lax
from jax.experimental import pallas as pl
from jax.experimental.pallas import tpu as pltpu
from jax.sharding import PartitionSpec as P


MESH = pl.DeviceIdType.MESH


def rms_scale(values, epsilon):
    return values * lax.rsqrt(jnp.mean(values * values, axis=-1, keepdims=True) + epsilon)


def attention_kernel(
    count,
    heads,
    query_ref,
    key_ref,
    value_ref,
    cos_ref,
    sin_ref,
    lambda_ref,
    head_gain_ref,
    residual_ref,
    mixer_gain_ref,
    channel_gain_ref,
    routes_ref,
    logits_ref,
    weight_hbm,
    stream_ref,
    normed_ref,
    place_ref,
    mix_ref,
    query_out,
    key_out,
    query_in,
    key_in,
    value_in,
    head_out,
    token_rows,
    projected,
    weight,
    w_sem,
    in_send,
    in_recv,
    out_send,
    out_recv,
):
    me = lax.axis_index("sp")
    tokens, model = query_ref.shape
    lanes = head_gain_ref.shape[1]
    map_dim = lanes // 2
    scale = map_dim ** (-0.5)
    load = pltpu.make_async_copy(weight_hbm, weight, w_sem)
    load.start()

    def sp_at(step):
        return {"sp": (me + step + count) % count}

    def columns(owner, h):
        return pl.ds(pl.multiple_of((owner * heads + h) * lanes, lanes), lanes)

    def far(k):
        return count // 2 + (k // 2) * (2 * (k % 2) - 1)

    def dest_columns(k, h):
        return columns((me + far(k)) % count, h)

    def remote(src, dst, send, recv, step):
        return pltpu.make_async_remote_copy(
            src_ref=src,
            dst_ref=dst,
            send_sem=send,
            recv_sem=recv,
            device_id=sp_at(step),
            device_id_type=MESH,
        )

    def inward(h, k, i):
        sources = (value_ref.at[:, dest_columns(k, h)], query_out.at[h, k], key_out.at[h, k])
        targets = (value_in.at[h, k], query_in.at[h, k], key_in.at[h, k])
        return remote(sources[i], targets[i], in_send.at[h, i, k], in_recv.at[h, i, k], far(k))

    def outward(h, k):
        return remote(
            head_out.at[h, k], token_rows.at[:, columns(me, h)], out_send.at[h, k], out_recv.at[h, k], -far(k)
        )

    barrier = pltpu.get_barrier_semaphore()
    for k in range(1, count):
        pl.semaphore_signal(barrier, inc=1, device_id=sp_at(k), device_id_type=MESH)

    first_half = lax.broadcasted_iota(jnp.int32, (tokens, lanes), 1) % map_dim < map_dim // 2

    def turned(ref, cols):
        x = ref[:, cols].astype(jnp.float32)
        ahead = pltpu.roll(x, lanes - map_dim // 2, 1)
        behind = pltpu.roll(x, map_dim // 2, 1)
        return x * cos_ref[...] + jnp.where(first_half, ahead, behind) * sin_ref[...]

    def prepare(h, cols):
        query = (turned(query_ref, cols) * scale).astype(jnp.bfloat16)
        key = turned(key_ref, cols).astype(jnp.bfloat16)
        return query, key

    for h in range(heads):
        query, key = prepare(h, columns(me, h))
        query_in[h, 0] = query
        key_in[h, 0] = key
        value_in[h, 0] = value_ref[:, columns(me, h)]

    pl.semaphore_wait(barrier, count - 1)

    for h in range(heads):

        @pl.loop(1, count)
        def _(k):
            inward(h, k, 0).start()

        @pl.loop(1, count)
        def _(k):
            query_out[h, k], key_out[h, k] = prepare(h, dest_columns(k, h))

        @pl.loop(1, count)
        def _(k):
            inward(h, k, 1).start()
            inward(h, k, 2).start()

    top = routes_ref.shape[1]
    capacity = mix_ref.shape[1] // count
    experts = lax.broadcasted_iota(jnp.int32, (tokens, 128), 1)
    places = lax.broadcasted_iota(jnp.int32, mix_ref.shape, 1)
    lower = lax.broadcasted_iota(jnp.int32, (tokens, tokens), 0)
    lower = (lower >= lax.broadcasted_iota(jnp.int32, (tokens, tokens), 1)).astype(jnp.bfloat16)
    logits = logits_ref[...]
    odds = jnp.exp(logits - jnp.max(logits, axis=-1, keepdims=True))
    shares = odds / jnp.sum(odds, axis=-1, keepdims=True)
    used = jnp.zeros((1, 128), jnp.float32)
    mix = jnp.zeros(mix_ref.shape, jnp.float32)
    place = jnp.zeros(mix_ref.shape, jnp.float32)
    for i in range(top):
        away = routes_ref[:, i : i + 1] - me
        away = jnp.where(away < 0, away + count, away)
        mid = count // 2
        ranked = jnp.where(away < mid, 2 * (mid - away), 2 * (away - mid) + 1)
        ranked = jnp.where(away == 0, 0, ranked)
        named = (experts == ranked).astype(jnp.float32)
        running = jnp.dot(lower, named.astype(jnp.bfloat16), preferred_element_type=jnp.float32)
        slot = jnp.sum(named * (running + used), axis=-1, keepdims=True).astype(jnp.int32) - 1
        used = used + jnp.sum(named, axis=0, keepdims=True)
        hit = places == ranked * capacity + slot
        mix = mix + jnp.where(hit, shares[:, i : i + 1], 0.0)
        place = place + jnp.where(hit, 1.0, 0.0)
    mix_ref[...] = mix
    place_ref[...] = place.astype(jnp.bfloat16)

    width = 2
    rows = width * tokens
    length = count * tokens
    in_first = lax.broadcasted_iota(jnp.int32, (rows, lanes), 1) < map_dim

    def part_of(total):
        return jnp.exp(total - jnp.max(total, axis=-1, keepdims=True))

    for h in range(heads):

        @pl.loop(1, count)
        def _(k):
            for i in range(3):
                inward(h, k, i).wait_recv()

        @pl.loop(0, count // width)
        def _(b):
            query = query_in[h, pl.ds(b * width, width)].reshape(rows, lanes).astype(jnp.float32)
            both = jnp.concatenate(
                [jnp.where(in_first, query, 0.0), jnp.where(in_first, 0.0, query)], axis=0
            ).astype(jnp.bfloat16)
            keys = key_in[h].reshape(length, lanes)
            scores = lax.dot_general(
                both, keys, (((1,), (1,)), ((), ())), preferred_element_type=jnp.float32
            )
            one, two = part_of(scores[:rows]), part_of(scores[rows:])
            one_scale = 1.0 / jnp.sum(one, axis=-1, keepdims=True)
            two_scale = lambda_ref[h] / jnp.sum(two, axis=-1, keepdims=True)
            mixing = (one * one_scale - two * two_scale).astype(jnp.bfloat16)
            mix = jnp.dot(
                mixing, value_in[h].reshape(length, lanes), preferred_element_type=jnp.float32
            )
            result = (rms_scale(mix, 1e-05) * head_gain_ref[...]).astype(jnp.bfloat16)
            head_out[h, pl.ds(b * width, width)] = result.reshape(width, tokens, lanes)
            for i in range(width):
                k = b * width + i

                @pl.when(k > 0)
                def _():
                    outward(h, k).start()

    for h in range(heads):
        token_rows[:, columns(me, h)] = head_out[h, 0]

    load.wait()
    for h in range(heads):

        @pl.loop(1, count)
        def _(k):
            outward(h, k).wait_recv()

    wide = math.gcd(model, 512)

    @pl.loop(0, model // wide)
    def _(n):
        cols = pl.ds(pl.multiple_of(n * wide, wide), wide)
        projected[:, cols] = jnp.dot(
            token_rows[...], weight[:, cols], preferred_element_type=jnp.float32
        )

    chunk = math.gcd(tokens, 16)

    @pl.loop(0, tokens // chunk)
    def _(n):
        part = pl.ds(pl.multiple_of(n * chunk, chunk), chunk)
        stream = residual_ref[part, :].astype(jnp.float32)
        stream = stream + rms_scale(projected[part, :], 1e-06) * mixer_gain_ref[...]
        stream = stream.astype(jnp.bfloat16)
        stream_ref[part, :] = stream
        normed = rms_scale(stream.astype(jnp.float32), 1e-06) * channel_gain_ref[...]
        normed_ref[part, :] = normed.astype(jnp.bfloat16)

    for h in range(heads):

        @pl.loop(1, count)
        def _(k):
            for i in range(3):
                inward(h, k, i).wait_send()
            outward(h, k).wait_send()


def attention_stage(
    queries,
    keys,
    values,
    lambdas,
    head_gain,
    out_weight,
    residual,
    mixer_gain,
    channel_gain,
    routes,
    logits,
):
    count = lax.axis_size("sp")
    heads = lambdas.shape[0]
    lanes = head_gain.shape[0]
    map_dim = lanes // 2
    tokens, model = residual.shape
    inverse = 1.0 / 10000.0 ** (jnp.arange(0, map_dim, 2, dtype=jnp.float32) / map_dim)
    positions = lax.axis_index("sp") * tokens + jnp.arange(tokens, dtype=jnp.int32)
    angles = positions.astype(jnp.float32)[:, None] * inverse[None, :]
    cosine, sine = jnp.cos(angles), jnp.sin(angles)
    cos_table = jnp.concatenate([cosine] * 4, axis=1)
    sin_table = jnp.concatenate([-sine, sine] * 2, axis=1)
    vmem = pl.BlockSpec(memory_space=pltpu.VMEM)
    smem = pl.BlockSpec(memory_space=pltpu.SMEM)
    half = jnp.bfloat16
    dma = pltpu.SemaphoreType.DMA
    blocks = pltpu.VMEM((heads, count, tokens, lanes), half)
    shape = jax.ShapeDtypeStruct((tokens, model), half)
    capacity = -(-max(2, 3 * tokens // count) // 16) * 16
    table = (tokens, count * capacity)
    return pl.pallas_call(
        functools.partial(attention_kernel, count, heads),
        out_shape=[
            shape,
            shape,
            jax.ShapeDtypeStruct(table, half),
            jax.ShapeDtypeStruct(table, jnp.float32),
        ],
        in_specs=[vmem] * 5 + [smem] + [vmem] * 6 + [pl.BlockSpec(memory_space=pl.ANY)],
        out_specs=[vmem] * 4,
        scratch_shapes=[
            blocks,
            blocks,
            blocks,
            blocks,
            blocks,
            blocks,
            pltpu.VMEM((tokens, heads * count * lanes), half),
            pltpu.VMEM((tokens, model), jnp.float32),
            pltpu.VMEM(out_weight.shape, half),
            dma,
            dma((heads, 3, count)),
            dma((heads, 3, count)),
            dma((heads, count)),
            dma((heads, count)),
        ],
        compiler_params=pltpu.CompilerParams(
            collective_id=2, has_side_effects=True, vmem_limit_bytes=60 * 1024 * 1024
        ),
        name="attention",
    )(
        queries,
        keys,
        values,
        cos_table,
        sin_table,
        lambdas,
        head_gain[None, :],
        residual,
        mixer_gain[None, :],
        channel_gain[None, :],
        routes,
        logits,
        out_weight,
    )


def expert_kernel(
    count,
    groups,
    rows_ref,
    place_ref,
    mix_ref,
    stream_ref,
    gain_ref,
    gate_hbm,
    up_hbm,
    down_hbm,
    out_ref,
    outgoing,
    arrived,
    own,
    pair_in,
    cross_in,
    final,
    returned,
    hidden,
    gate_w,
    up_w,
    down_w,
    w_sem,
    a_send,
    a_recv,
    b_send,
    b_recv,
    c_send,
    c_recv,
    d_send,
    d_recv,
    e_send,
    e_recv,
    f_send,
    f_recv,
):
    me = lax.axis_index("sp")
    dp = lax.axis_index("dp")
    chip, core = dp // 2, dp % 2
    other = {"sp": me, "dp": chip * 2 + (1 - core)}

    def chip_at(step):
        return {"sp": me, "dp": ((chip + step + groups) % groups) * 2 + core}

    def far(k):
        return count // 2 + (k // 2) * (2 * (k % 2) - 1)

    def sp_at(step):
        return {"sp": (me + step + count) % count, "dp": dp}

    def remote(src, dst, send, recv, device):
        return pltpu.make_async_remote_copy(
            src_ref=src, dst_ref=dst, send_sem=send, recv_sem=recv, device_id=device, device_id_type=MESH
        )

    def send_out(k):
        return remote(outgoing.at[k], arrived.at[k, 0, 0], a_send.at[k], a_recv.at[k], sp_at(far(k)))

    def cross_out(k, j):
        return remote(arrived.at[k, 0, 0], arrived.at[k, 0, j], b_send.at[k, j], b_recv.at[k, j], chip_at(j))

    def twin_out(k, j):
        return remote(arrived.at[k, 0, j], arrived.at[k, 1, j], c_send.at[k, j], c_recv.at[k, j], other)

    def pair_out(k):
        return remote(arrived.at[k, 1], pair_in.at[k], d_send.at[k], d_recv.at[k], other)

    def cross_back(k, j):
        return remote(own.at[k, j], cross_in.at[k, j], e_send.at[k, j], e_recv.at[k, j], chip_at(-j))

    def send_back(k):
        return remote(final.at[k], returned.at[k], f_send.at[k], f_recv.at[k], sp_at(-far(k)))

    weights = [
        pltpu.make_async_copy(hbm, vmem, w_sem.at[i])
        for i, (hbm, vmem) in enumerate(((gate_hbm, gate_w), (up_hbm, up_w), (down_hbm, down_w)))
    ]
    for copy in weights:
        copy.start()

    barrier = pltpu.get_barrier_semaphore()
    peers = [sp_at(k) for k in range(1, count)] + [chip_at(j) for j in range(1, groups)] + [other]
    for peer in peers:
        pl.semaphore_signal(barrier, inc=1, device_id=peer, device_id_type=MESH)

    capacity = outgoing.shape[1]
    model = rows_ref.shape[1]
    units = gate_w.shape[1]
    wide = math.gcd(model, 512)

    @pl.loop(0, model // wide)
    def _(n):
        cols = pl.ds(pl.multiple_of(n * wide, wide), wide)
        block = lax.dot_general(
            place_ref[...], rows_ref[:, cols], (((0,), (0,)), ((), ())), preferred_element_type=jnp.float32
        )
        block = block.astype(jnp.bfloat16).reshape(count, capacity, wide)
        arrived[0, 0, 0, :, cols] = block[0]
        outgoing[:, :, cols] = block

    pl.semaphore_wait(barrier, len(peers))

    @pl.loop(1, count)
    def _(k):
        send_out(k).start()

    width = 1
    rounds = count // width

    def per_k(group, action):
        for i in range(width):
            action(group * width + i)

    def forward(k):
        @pl.when(k > 0)
        def _():
            send_out(k).wait_recv()

        for j in range(1, groups):
            cross_out(k, j).start()
        twin_out(k, 0).start()

    def forward_twin(k):
        for j in range(1, groups):
            cross_out(k, j).wait_recv()
            twin_out(k, j).start()

    def complete(k):
        for j in range(groups):
            twin_out(k, j).wait_recv()

    def pair_sum(k):
        pair_out(k).wait_recv()
        for j in range(groups):
            own[k, j] = (own[k, j].astype(jnp.float32) + pair_in[k, j].astype(jnp.float32)).astype(jnp.bfloat16)
        for j in range(1, groups):
            cross_back(k, j).start()

    def total(k):
        value = own[k, 0].astype(jnp.float32)
        for j in range(1, groups):
            cross_back(k, j).wait_recv()
            value = value + cross_in[k, j].astype(jnp.float32)
        value = value.astype(jnp.bfloat16)

        @pl.when(k > 0)
        def _():
            final[k] = value
            send_back(k).start()

        @pl.when(k == 0)
        def _():
            returned[k] = value

    tile = math.gcd(units, 256)

    def compute(group):
        first = group * width
        held = width * 2 * groups * capacity
        slab = arrived.at[pl.ds(first, width)]

        @pl.loop(0, units // tile)
        def _(n):
            cols = pl.ds(pl.multiple_of(n * tile, tile), tile)
            value = slab[...].reshape(held, model)
            gate = jnp.dot(value, gate_w[:, cols], preferred_element_type=jnp.float32)
            up = jnp.dot(value, up_w[:, cols], preferred_element_type=jnp.float32)
            hidden[:, cols] = (gate / (1.0 + jnp.exp(-gate)) * up).astype(jnp.bfloat16)

        @pl.loop(0, model // wide)
        def _(n):
            cols = pl.ds(pl.multiple_of(n * wide, wide), wide)
            part = jnp.dot(hidden[...], down_w[:, cols], preferred_element_type=jnp.float32)
            part = part.astype(jnp.bfloat16).reshape(width, 2, groups, capacity, wide)
            for i in range(width):
                own[first + i, :, :, cols] = part[i, 0]
                arrived[first + i, 1, :, :, cols] = part[i, 1]

        per_k(group, lambda k: pair_out(k).start())

    @pl.loop(0, rounds + 3)
    def _(g):
        @pl.when(g < rounds)
        def _():
            per_k(g, forward)

        @pl.when((g >= 2) & (g < rounds + 2))
        def _():
            per_k(g - 2, pair_sum)

        @pl.when(g >= 3)
        def _():
            per_k(g - 3, total)

        @pl.when((g >= 1) & (g < rounds + 1))
        def _():
            @pl.when(g == 1)
            def _():
                for copy in weights:
                    copy.wait()

            per_k(g - 1, forward_twin)
            per_k(g - 1, complete)
            compute(g - 1)

    @pl.loop(1, count)
    def _(k):
        send_back(k).wait_recv()

    square = jnp.zeros((stream_ref.shape[0], 1), jnp.float32)
    share = mix_ref[...]
    high = share.astype(jnp.bfloat16)
    low = (share - high.astype(jnp.float32)).astype(jnp.bfloat16)
    pieces = []
    for n in range(model // wide):
        cols = slice(n * wide, (n + 1) * wide)
        back = returned[:, :, cols].reshape(count * capacity, wide)
        piece = jnp.dot(high, back, preferred_element_type=jnp.float32)
        piece = piece + jnp.dot(low, back, preferred_element_type=jnp.float32)
        square = square + jnp.sum(piece * piece, axis=-1, keepdims=True)
        pieces.append(piece)
    norm = lax.rsqrt(square / model + 1e-06)
    for n, piece in enumerate(pieces):
        cols = slice(n * wide, (n + 1) * wide)
        value = stream_ref[:, cols].astype(jnp.float32) + piece * norm * gain_ref[:, cols]
        out_ref[:, cols] = value.astype(jnp.bfloat16)

    @pl.loop(0, count)
    def _(k):
        @pl.when(k > 0)
        def _():
            send_out(k).wait_send()
            send_back(k).wait_send()

        for j in range(1, groups):
            cross_out(k, j).wait_send()
            cross_back(k, j).wait_send()
        for j in range(groups):
            twin_out(k, j).wait_send()
        pair_out(k).wait_send()


def expert_stage(normed, stream, place, mix, expert_gain, gate_weight, up_weight, down_weight):
    count, dp_count = lax.axis_size("sp"), lax.axis_size("dp")
    groups = dp_count // 2
    tokens, model = normed.shape
    units = gate_weight.shape[1]
    capacity = mix.shape[1] // count
    vmem, anywhere = pl.BlockSpec(memory_space=pltpu.VMEM), pl.BlockSpec(memory_space=pl.ANY)
    half = jnp.bfloat16
    dma = pltpu.SemaphoreType.DMA
    return pl.pallas_call(
        functools.partial(expert_kernel, count, groups),
        out_shape=jax.ShapeDtypeStruct((tokens, model), jnp.bfloat16),
        in_specs=[vmem] * 5 + [anywhere] * 3,
        out_specs=vmem,
        scratch_shapes=[
            pltpu.VMEM((count, capacity, model), half),
            pltpu.VMEM((count, 2, groups, capacity, model), half),
            pltpu.VMEM((count, groups, capacity, model), half),
            pltpu.VMEM((count, groups, capacity, model), half),
            pltpu.VMEM((count, groups, capacity, model), half),
            pltpu.VMEM((count, capacity, model), half),
            pltpu.VMEM((count, capacity, model), half),
            pltpu.VMEM((2 * groups * capacity, units), half),
            pltpu.VMEM((model, units), half),
            pltpu.VMEM((model, units), half),
            pltpu.VMEM((units, model), half),
            dma((3,)),
            dma((count,)),
            dma((count,)),
            dma((count, groups)),
            dma((count, groups)),
            dma((count, groups)),
            dma((count, groups)),
            dma((count,)),
            dma((count,)),
            dma((count, groups)),
            dma((count, groups)),
            dma((count,)),
            dma((count,)),
        ],
        compiler_params=pltpu.CompilerParams(
            collective_id=1, has_side_effects=True, vmem_limit_bytes=67043328
        ),
        name="experts",
    )(normed, place, mix, stream, expert_gain[None, :], gate_weight, up_weight, down_weight)


def local(
    queries,
    key_rows,
    value_rows,
    lambdas,
    head_gain,
    out_weight,
    residual,
    mixer_gain,
    channel_gain,
    expert_gain,
    routes,
    route_logits,
    gate_weight,
    up_weight,
    down_weight,
):
    stream, normed, place, mix = attention_stage(
        queries[0],
        key_rows[0],
        value_rows[0],
        lambdas,
        head_gain,
        out_weight,
        residual[0],
        mixer_gain,
        channel_gain,
        routes[0],
        route_logits[0],
    )
    updated = expert_stage(
        normed,
        stream,
        place,
        mix,
        expert_gain,
        gate_weight[0],
        up_weight[0],
        down_weight[0],
    )
    return updated[None]


def solution(mesh):
    placed = (
        P("dp", "sp", None),
        P("dp", "sp", None),
        P("dp", "sp", None),
        P("sp"),
        P(),
        P(),
        P("dp", "sp", None),
        P(),
        P(),
        P(),
        P("dp", "sp", None),
        P("dp", "sp", None),
        P("sp", None, "dp"),
        P("sp", None, "dp"),
        P("sp", "dp", None),
    )
    return jax.shard_map(
        local, mesh=mesh, in_specs=placed, out_specs=P("dp", "sp", None), check_vma=False
    )
```
